32 devices in a mesh: grp: 2 (over y), ra: 4 (over z), cb: 4 (over x, core).
Axes of the slice: x: 2, y: 2, z: 4, core: 2. Of those that a mesh axis runs over, the one named last changes fastest.
Arguments:
- tokens: bfloat16 [512, 4096], P('grp', 'ra'), parts along dimension 0, may hold values from -30 to 30, as said below
- norm_gain: bfloat16 [4096], P('ra'), may hold values from 0.099609375 to 1.8984375
- w_gate: bfloat16 [4096, 11264], P('ra', 'cb'), may hold values from -0.09375 to 0.09375
- w_value: bfloat16 [4096, 11264], P('ra', 'cb'), may hold values from -0.09375 to 0.09375
- conv_gate: float32 [3, 11264], P(None, 'cb'), may hold values from -3 to 3
- conv_value: float32 [3, 11264], P(None, 'cb'), may hold values from -3 to 3
- bias_gate: float32 [11264], P('cb'), may hold values from -3 to 3
- bias_value: float32 [11264], P('cb'), may hold values from -3 to 3
- w_down: bfloat16 [11264, 4096], P('cb', 'ra'), may hold values from -1 to 1
- out_gain: bfloat16 [4096], P('ra'), may hold values from 0.099609375 to 1.8984375
Outputs:
- normed_out: bfloat16 [512, 4096], P('grp', 'ra'), parts along dimension 0
The draws below stay inside these ranges and needn't reach their ends.
There are 2 independent parts, one for each index of `grp`. The reference program is written for one: setup_inputs(seed, part) draws one part's arguments, and reference() takes and returns one part's arrays. A program takes and returns all parts, laid end to end along the dimension named above; an argument that names none is the same for every part. Nothing has to cross between parts.
Inputs may be any that keep to these rules, and one draw needn't show every extreme that they name: `tokens`: feature scales differ along the width.
All inputs are finite; a program needn't handle non-finite values.
Results may differ from the reference program's by a relative error of at most 0.0059.
Values may be sent and summed in bfloat16 or wider, within the bound.
A program may use at most 64 MiB of HBM per device.

```python
import jax
import jax.numpy as jnp
from jax import lax

D = 4096
FF = 11264
TOKENS = 256


def draw_tokens(key, part):
    first_key, second_key, third_key = jax.random.split(jax.random.fold_in(key, 11), 3)
    columns = jnp.arange(D, dtype=jnp.float32) / D
    rough = jax.random.uniform(second_key, (D,), jnp.float32, 0.6, 1.5)
    row_scales = jnp.exp(jax.random.uniform(third_key, (TOKENS, 1), jnp.float32, -0.5, 0.5))
    values = jnp.clip(jax.random.normal(first_key, (TOKENS, D), jnp.float32), -4.0, 4.0)
    scales = 0.6 * 3.0 ** columns * rough
    return (values * scales * row_scales).astype(jnp.bfloat16)


def draw_w_down(key, part):
    own_key, pattern_key, sign_key, size_key = jax.random.split(jax.random.fold_in(key, 23), 4)
    own = jnp.clip(jax.random.normal(own_key, (FF, D), jnp.float32), -4.0, 4.0)
    pattern = jnp.clip(jax.random.normal(pattern_key, (D,), jnp.float32), -3.0, 3.0)
    signs = jnp.where(jax.random.randint(sign_key, (FF, 1), 0, 2) == 0, -1.0, 1.0).astype(jnp.float32)
    sizes = jax.random.uniform(size_key, (FF, 1), jnp.float32, 0.5, 1.5)
    mixed = 0.866 * own + 0.5 * signs * sizes * pattern[None, :]
    return (mixed / jnp.sqrt(jnp.float32(FF))).astype(jnp.bfloat16)


def shard_levels(rng, shape, cuts, low, top_value):
    factor_of, own = 1.0, jax.random.fold_in(rng, 6)
    for dim, shards_of in cuts:
        draws = jnp.exp(jax.random.uniform(jax.random.fold_in(own, dim), (shards_of,), jnp.float32, low / len(cuts), top_value / len(cuts)))
        factor_of = factor_of * jnp.repeat(draws, shape[dim] // shards_of).reshape([-1 if axis == dim else 1 for axis in range(len(shape))])
    return factor_of


def centred(key, extent, scale, most, pieces=(), kind=jnp.bfloat16):
    drawn = jax.random.normal(key, extent, jnp.float32) * scale
    if len(pieces) > 0:
        drawn = shard_levels(key, extent, pieces, -0.22, 0.18) * drawn
    return jnp.clip(drawn, min=-most, max=most).astype(kind)


def setup_inputs(seed: int = 0, part: int = 0) -> dict:
    streams_of = jax.random.split(jax.random.key(seed), 11)
    part_splits = jax.random.split(jax.random.fold_in(streams_of[10], part), 11)
    return {
        "tokens": draw_tokens(jax.random.fold_in(jax.random.fold_in(streams_of[10], part), 71), part),
        "norm_gain": jnp.clip(1.0 + 0.18 * jax.random.normal(streams_of[1], (D,), jnp.float32), 0.099609375, 1.8984375).astype(jnp.bfloat16),
        "w_gate": centred(streams_of[2], (D, FF), D ** -0.5, 0.09375, ((0, 4), (1, 4))),
        "w_value": centred(streams_of[3], (D, FF), D ** -0.5, 0.09375, ((0, 4), (1, 4))),
        "conv_gate": centred(streams_of[4], (3, FF), 0.58, 3.0, ((1, 4),), jnp.float32),
        "conv_value": centred(streams_of[5], (3, FF), 0.58, 3.0, ((1, 4),), jnp.float32),
        "bias_gate": centred(streams_of[6], (FF,), 0.5, 3.0, ((0, 4),), jnp.float32),
        "bias_value": centred(streams_of[7], (FF,), 0.5, 3.0, ((0, 4),), jnp.float32),
        "w_down": draw_w_down(jax.random.fold_in(streams_of[10], 71), part),
        "out_gain": jnp.clip(1.0 + 0.18 * jax.random.normal(streams_of[9], (D,), jnp.float32), 0.099609375, 1.8984375).astype(jnp.bfloat16),
    }


EPSILON = 1e-06
RESIDUAL_WEIGHT = 0.25

def spread(signal, kernel):
    padded = jnp.pad(signal, ((1, 1), (0, 0)))
    return padded[:-2] * kernel[0] + padded[1:-1] * kernel[1] + padded[2:] * kernel[2]

def reference(tokens, norm_gain, w_gate, w_value, conv_gate, conv_value, bias_gate, bias_value, w_down, out_gain):
    wide_in = tokens.astype(jnp.float32)
    rscale = lax.rsqrt(lax.optimization_barrier(jnp.mean(wide_in * wide_in, axis=1, keepdims=True)) + EPSILON)
    normed = (wide_in * rscale * norm_gain.astype(jnp.float32)).astype(jnp.bfloat16)
    gate_sum = jnp.dot(normed, w_gate, preferred_element_type=jnp.float32)
    value_sum = jnp.dot(normed, w_value, preferred_element_type=jnp.float32)
    gate_conv = spread(gate_sum, conv_gate) + bias_gate
    value_conv = spread(value_sum, conv_value) + bias_value
    hidden = (jax.nn.silu(gate_conv) * value_conv).astype(jnp.bfloat16)
    branch = jnp.dot(hidden, w_down, preferred_element_type=jnp.float32)
    summed = RESIDUAL_WEIGHT * wide_in + branch
    oscale = lax.rsqrt(lax.optimization_barrier(jnp.mean(summed * summed, axis=1, keepdims=True)) + EPSILON)
    return (summed * oscale * out_gain.astype(jnp.float32)).astype(jnp.bfloat16)
```

```python
import functools

import jax
import jax.numpy as jnp
from jax import lax
from jax.experimental import pallas as pl
from jax.experimental.pallas import tpu as pltpu
from jax.sharding import PartitionSpec as P

EPSILON = 1e-06
RESIDUAL_WEIGHT = 0.25
MESH = pl.DeviceIdType.MESH
LANES = 128
SKEW = 2
PIECES = 4


def spread(signal, kernel):
    padded = jnp.pad(signal, ((1, 1), (0, 0)))
    return padded[:-2] * kernel[0] + padded[1:-1] * kernel[1] + padded[2:] * kernel[2]


def activate(gate_sum, value_sum, kernel_gate, kernel_value, offset_gate, offset_value):
    gate_conv = spread(gate_sum, kernel_gate) + offset_gate
    value_conv = spread(value_sum, kernel_value) + offset_value
    return (jax.nn.silu(gate_conv) * value_conv).astype(jnp.bfloat16)


def plain_body(
    tokens,
    norm_gain,
    w_gate,
    w_value,
    conv_gate,
    conv_value,
    bias_gate,
    bias_value,
    w_down,
    out_gain,
):
    wide_in = tokens.astype(jnp.float32)
    width = wide_in.shape[1] * lax.axis_size("ra")
    squares = lax.psum(jnp.sum(wide_in * wide_in, axis=1), "ra")
    rscale = lax.rsqrt(squares / width + EPSILON)
    normed = (wide_in * rscale[:, None] * norm_gain.astype(jnp.float32)).astype(jnp.bfloat16)
    part_gate = jnp.dot(normed, w_gate, preferred_element_type=jnp.float32)
    part_value = jnp.dot(normed, w_value, preferred_element_type=jnp.float32)
    gate_sum, value_sum = (
        lax.psum_scatter(part_gate, "ra", scatter_dimension=1, tiled=True),
        lax.psum_scatter(part_value, "ra", scatter_dimension=1, tiled=True),
    )
    share_cols = gate_sum.shape[1]
    first_col = lax.axis_index("ra") * share_cols
    local_hidden = activate(
        gate_sum,
        value_sum,
        lax.dynamic_slice_in_dim(conv_gate, first_col, share_cols, 1),
        lax.dynamic_slice_in_dim(conv_value, first_col, share_cols, 1),
        lax.dynamic_slice_in_dim(bias_gate, first_col, share_cols, 0),
        lax.dynamic_slice_in_dim(bias_value, first_col, share_cols, 0),
    )
    partial_value = jnp.dot(
        lax.all_gather(local_hidden, "ra", axis=1, tiled=True),
        w_down,
        preferred_element_type=jnp.float32,
    )
    branch = lax.psum(partial_value, "cb")
    summed = RESIDUAL_WEIGHT * wide_in + branch
    totals = lax.psum(jnp.sum(summed * summed, axis=1), "ra")
    oscale = lax.rsqrt(totals / width + EPSILON)
    return (summed * oscale[:, None] * out_gain.astype(jnp.float32)).astype(jnp.bfloat16)


def to_row(column):
    rows = column.shape[0]
    return jnp.transpose(jnp.broadcast_to(column, (rows, LANES)))[:8]


def to_column(row):
    return jnp.transpose(jnp.broadcast_to(row, (LANES, row.shape[1])))[:, :1]


def shifted_sum(signal, taps, offset):
    rows = signal.shape[0]
    index = lax.broadcasted_iota(jnp.int32, signal.shape, 0)
    before = jnp.where(index == 0, 0.0, pltpu.roll(signal, 1, 0))
    after = jnp.where(index == rows - 1, 0.0, pltpu.roll(signal, rows - 1, 0))
    return before * taps[0:1] + signal * taps[1:2] + after * taps[2:3] + offset


def kernel(
    ra_size,
    tokens,
    norm_gain,
    w_gate,
    w_value,
    conv_gate,
    conv_value,
    bias_gate,
    bias_value,
    w_down,
    out_gain,
    out,
    w_in,
    w_out,
    normed,
    rs_out,
    rs_in,
    hid,
    acc,
    pair_in,
    x_out,
    x_in,
    summed,
    sq_col,
    sq_first,
    sq_last,
    w_in_sem,
    w_out_sem,
    rs_send,
    rs_recv,
    hid_send,
    hid_recv,
    pair_send,
    pair_recv,
    x_send,
    x_recv,
    sum_send,
    sum_recv,
    first_send,
    first_recv,
    last_send,
    last_recv,
):
    rows, wide = tokens.shape
    chunks = hid.shape[0]
    half = wide // 2
    width = wide * ra_size
    piece = rows // PIECES
    last = ra_size - 1

    me = lax.axis_index("ra")
    cb = lax.axis_index("cb")
    core = lax.rem(cb, 2)
    partner = cb + 1 - 2 * core
    across = lax.rem(cb + 2, 4)

    place = (me, last - me)
    ahead = (lax.rem(me + 1, ra_size), lax.rem(me + last, ra_size))
    behind = (ahead[1], ahead[0])
    lanes = (slice(LANES, 2 * LANES), slice(0, LANES))

    def w_in_copies(chunk):
        cols = pl.ds(pl.multiple_of(chunk * LANES, LANES), LANES)
        return [
            pltpu.make_async_copy(
                w.at[:, cols], w_in.at[chunk, :, n * LANES : (n + 1) * LANES], w_in_sem.at[n, chunk]
            )
            for n, w in enumerate((w_gate, w_value))
        ]

    def w_out_copies(k):
        return [
            pltpu.make_async_copy(
                w_down.at[pl.ds(pl.multiple_of((k + n * chunks) * LANES, LANES), LANES), :],
                w_out.at[k, n * LANES : (n + 1) * LANES, :],
                w_out_sem.at[n, k],
            )
            for n in range(2)
        ]

    def rs_copy(d, k):
        return pltpu.make_async_remote_copy(
            src_ref=rs_out.at[d, k],
            dst_ref=rs_in.at[d, k],
            send_sem=rs_send.at[d, k],
            recv_sem=rs_recv.at[d, k],
            device_id={"ra": ahead[d]},
            device_id_type=MESH,
        )

    def hid_copy(d, k):
        return pltpu.make_async_remote_copy(
            src_ref=hid.at[k, :, lanes[d]],
            dst_ref=hid.at[k, :, lanes[d]],
            send_sem=hid_send.at[d, k],
            recv_sem=hid_recv.at[d, k],
            device_id={"ra": behind[d]},
            device_id_type=MESH,
        )

    barrier = pltpu.get_barrier_semaphore()
    for step in range(1, ra_size):
        for q in (cb, partner):
            pl.semaphore_signal(
                barrier, inc=1, device_id={"ra": lax.rem(me + step, ra_size), "cb": q}, device_id_type=MESH
            )
    for q in (partner, across):
        pl.semaphore_signal(barrier, inc=1, device_id={"cb": q}, device_id_type=MESH)

    @pl.loop(0, chunks)
    def _(k):
        for chunk in (k, k + chunks):
            for copy in w_in_copies(chunk):
                copy.start()

    @pl.loop(0, chunks)
    def _(k):
        for copy in w_out_copies(k):
            copy.start()

    wide_in = tokens[...].astype(jnp.float32)
    sq_first[me] = to_row(jnp.sum(wide_in * wide_in, axis=1, keepdims=True))
    acc[...] = jnp.zeros_like(acc)
    pl.semaphore_wait(barrier, 2 * last + 2)

    def first_copy(step):
        return pltpu.make_async_remote_copy(
            src_ref=sq_first.at[me],
            dst_ref=sq_first.at[me],
            send_sem=first_send.at[step],
            recv_sem=first_recv.at[me],
            device_id={"ra": lax.rem(me + step, ra_size)},
            device_id_type=MESH,
        )

    for step in range(1, ra_size):
        first_copy(step).start()
    for step in range(1, ra_size):
        source = lax.rem(me + step, ra_size)
        pltpu.make_async_remote_copy(
            src_ref=sq_first.at[source],
            dst_ref=sq_first.at[source],
            send_sem=first_send.at[step],
            recv_sem=first_recv.at[source],
            device_id={"ra": source},
            device_id_type=MESH,
        ).wait_recv()
    squares = sq_first[0, 0:1]
    for n in range(1, ra_size):
        squares = squares + sq_first[n, 0:1]
    rscale = lax.rsqrt(to_column(squares) / width + EPSILON)
    normed[...] = (tokens[...].astype(jnp.float32) * rscale * norm_gain[...].astype(jnp.float32)).astype(
        jnp.bfloat16
    )

    def reduce_step(d, k):
        chunk = k + chunks if d == 0 else k
        for copy in w_in_copies(chunk):
            copy.wait()
        part = jnp.dot(normed[...], w_in[chunk], preferred_element_type=jnp.float32)

        @pl.when(place[d] == 0)
        def _():
            rs_out[d, k] = part.astype(jnp.bfloat16)
            rs_copy(d, k).start()

        @pl.when(place[d] > 0)
        def _():
            rs_copy(d, k).wait_recv()
            total = part + rs_in[d, k].astype(jnp.float32)

            @pl.when(place[d] < last)
            def _():
                rs_out[d, k] = total.astype(jnp.bfloat16)
                rs_copy(d, k).start()

            @pl.when(place[d] == last)
            def _():
                cols = pl.ds(pl.multiple_of(chunk * LANES, LANES), LANES)
                gate = shifted_sum(total[:, :LANES], conv_gate[:, cols], bias_gate[:, cols])
                value = shifted_sum(total[:, LANES:], conv_value[:, cols], bias_value[:, cols])
                hid[k, :, lanes[d]] = (gate / (1.0 + jnp.exp(-gate)) * value).astype(jnp.bfloat16)
                hid_copy(d, k).start()

    def down_step(k):
        for copy in w_out_copies(k):
            copy.wait()
        for n in range(2):
            acc[n] += jnp.dot(
                hid[k], w_out[k, :, n * half : (n + 1) * half], preferred_element_type=jnp.float32
            )

    @pl.loop(0, chunks + 2 * SKEW * last)
    def _(i):
        for d in range(2):
            k = i - SKEW * place[d]
            pl.when((k >= 0) & (k < chunks))(functools.partial(reduce_step, d, k))
        for d in range(2):
            k = i - SKEW * (2 * last - place[d])

            @pl.when((k >= 0) & (k < chunks) & (place[d] < last))
            def _():
                hid_copy(d, k).wait_recv()

                @pl.when(place[d] > 0)
                def _():
                    hid_copy(d, k).start()

        k = i - SKEW * (last + jnp.maximum(place[0], place[1]))
        pl.when((k >= 0) & (k < chunks))(functools.partial(down_step, k))

    def rows_of(p):
        return pl.ds(p * piece, piece)

    def pair_copy(p):
        return pltpu.make_async_remote_copy(
            src_ref=acc.at[1 - core, rows_of(p)],
            dst_ref=pair_in.at[rows_of(p)],
            send_sem=pair_send.at[p],
            recv_sem=pair_recv.at[p],
            device_id={"cb": partner},
            device_id_type=MESH,
        )

    def x_copy(p):
        return pltpu.make_async_remote_copy(
            src_ref=x_out.at[rows_of(p)],
            dst_ref=x_in.at[rows_of(p)],
            send_sem=x_send.at[p],
            recv_sem=x_recv.at[p],
            device_id={"cb": across},
            device_id_type=MESH,
        )

    def sum_copy(p, n):
        return pltpu.make_async_remote_copy(
            src_ref=summed.at[n, rows_of(p)],
            dst_ref=summed.at[n, rows_of(p)],
            send_sem=sum_send.at[p],
            recv_sem=sum_recv.at[p],
            device_id={"cb": partner},
            device_id_type=MESH,
        )

    def last_copy(owner, n, ra, q):
        return pltpu.make_async_remote_copy(
            src_ref=sq_last.at[owner],
            dst_ref=sq_last.at[owner],
            send_sem=last_send.at[n],
            recv_sem=last_recv.at[owner],
            device_id={"ra": ra, "cb": q},
            device_id_type=MESH,
        )

    for p in range(PIECES):
        pair_copy(p).start()
    for p in range(PIECES):
        pair_copy(p).wait_recv()
        x_out[rows_of(p), :] = (acc[core, rows_of(p)] + pair_in[rows_of(p), :]).astype(jnp.bfloat16)
        x_copy(p).start()
    own_cols = pl.ds(pl.multiple_of(core * half, LANES), half)
    for p in range(PIECES):
        x_copy(p).wait_recv()
        branch = x_out[rows_of(p), :].astype(jnp.float32) + x_in[rows_of(p), :].astype(jnp.float32)
        total = RESIDUAL_WEIGHT * tokens[rows_of(p), own_cols].astype(jnp.float32) + branch
        summed[core, rows_of(p)] = total
        sum_copy(p, core).start()
        sq_col[rows_of(p), :] = jnp.broadcast_to(jnp.sum(total * total, axis=1, keepdims=True), (piece, LANES))

    mine = 2 * me + core
    sq_last[mine] = jnp.transpose(sq_col[...])[:8]
    targets = [(me, partner)]
    for step in range(1, ra_size):
        targets += [(lax.rem(me + step, ra_size), q) for q in (cb, partner)]
    for n, (ra, q) in enumerate(targets):
        last_copy(mine, n, ra, q).start()
    for p in range(PIECES):
        sum_copy(p, 1 - core).wait_recv()
    for n, (ra, q) in enumerate(targets):
        last_copy(2 * ra + lax.rem(q, 2), n, ra, q).wait_recv()
    totals = sq_last[0, 0:1]
    for n in range(1, 2 * ra_size):
        totals = totals + sq_last[n, 0:1]
    oscale = lax.rsqrt(to_column(totals) / width + EPSILON)
    for n in range(2):
        cols = slice(n * half, (n + 1) * half)
        out[:, cols] = (summed[n] * oscale * out_gain[:, cols].astype(jnp.float32)).astype(jnp.bfloat16)

    for step in range(1, ra_size):
        first_copy(step).wait_send()
    for d in range(2):

        @pl.loop(0, chunks)
        def _(k):
            @pl.when(place[d] < last)
            def _():
                rs_copy(d, k).wait_send()

            @pl.when(place[d] > 0)
            def _():
                hid_copy(d, k).wait_send()

    for p in range(PIECES):
        pair_copy(p).wait_send()
        x_copy(p).wait_send()
        sum_copy(p, core).wait_send()
    for n, (ra, q) in enumerate(targets):
        last_copy(mine, n, ra, q).wait_send()


def fused_body(
    tokens,
    norm_gain,
    w_gate,
    w_value,
    conv_gate,
    conv_value,
    bias_gate,
    bias_value,
    w_down,
    out_gain,
):
    ra_size = lax.axis_size("ra")
    rows, wide = tokens.shape
    chunks = w_gate.shape[1] // (2 * LANES)
    vmem = pl.BlockSpec(memory_space=pltpu.VMEM)
    anywhere = pl.BlockSpec(memory_space=pl.ANY)
    f32, bf16 = jnp.float32, jnp.bfloat16
    dma = pltpu.SemaphoreType.DMA
    return pl.pallas_call(
        functools.partial(kernel, ra_size),
        out_shape=jax.ShapeDtypeStruct((rows, wide), bf16),
        in_specs=[vmem, vmem, anywhere, anywhere, vmem, vmem, vmem, vmem, anywhere, vmem],
        out_specs=vmem,
        scratch_shapes=[
            pltpu.VMEM((2 * chunks, wide, 2 * LANES), bf16),
            pltpu.VMEM((chunks, 2 * LANES, wide), bf16),
            pltpu.VMEM((rows, wide), bf16),
            pltpu.VMEM((2, chunks, rows, 2 * LANES), bf16),
            pltpu.VMEM((2, chunks, rows, 2 * LANES), bf16),
            pltpu.VMEM((chunks, rows, 2 * LANES), bf16),
            pltpu.VMEM((2, rows, wide // 2), f32),
            pltpu.VMEM((rows, wide // 2), f32),
            pltpu.VMEM((rows, wide // 2), bf16),
            pltpu.VMEM((rows, wide // 2), bf16),
            pltpu.VMEM((2, rows, wide // 2), f32),
            pltpu.VMEM((rows, LANES), f32),
            pltpu.VMEM((ra_size, 8, rows), f32),
            pltpu.VMEM((2 * ra_size, 8, rows), f32),
            dma((2, 2 * chunks)),
            dma((2, chunks)),
            dma((2, chunks)),
            dma((2, chunks)),
            dma((2, chunks)),
            dma((2, chunks)),
            dma((PIECES,)),
            dma((PIECES,)),
            dma((PIECES,)),
            dma((PIECES,)),
            dma((PIECES,)),
            dma((PIECES,)),
            dma((ra_size,)),
            dma((ra_size,)),
            dma((2 * ra_size,)),
            dma((2 * ra_size,)),
        ],
        compiler_params=pltpu.CompilerParams(
            collective_id=0, has_side_effects=True, vmem_limit_bytes=56 * 1024 * 1024
        ),
    )(
        tokens,
        norm_gain.reshape(1, -1),
        w_gate,
        w_value,
        conv_gate,
        conv_value,
        bias_gate.reshape(1, -1),
        bias_value.reshape(1, -1),
        w_down,
        out_gain.reshape(1, -1),
    )


def solution(mesh):
    ra_size, cb_size = mesh.shape["ra"], mesh.shape["cb"]

    def body(*args):
        rows, wide = args[0].shape
        hidden = args[2].shape[1]
        fits = (
            ra_size >= 2
            and cb_size == 4
            and rows % LANES == 0
            and wide % (2 * LANES) == 0
            and hidden % (2 * LANES) == 0
            and 3 * 2 * wide * hidden + 10 * rows * hidden + 20 * rows * wide < 48 * 1024 * 1024
        )
        return fused_body(*args) if fits else plain_body(*args)

    return jax.shard_map(
        body,
        mesh=mesh,
        in_specs=(
            P("grp", "ra"),
            P("ra"),
            P("ra", "cb"),
            P("ra", "cb"),
            P(None, "cb"),
            P(None, "cb"),
            P("cb"),
            P("cb"),
            P("cb", "ra"),
            P("ra"),
        ),
        out_specs=P("grp", "ra"),
        check_vma=False,
    )
```

```python
import functools

import jax
import jax.numpy as jnp
from jax import lax
from jax.experimental import pallas as pl
from jax.experimental.pallas import tpu as pltpu
from jax.sharding import PartitionSpec as P

EPSILON = 1e-06
RESIDUAL_WEIGHT = 0.25
MESH = pl.DeviceIdType.MESH
LANES = 128
LEAD = 8
SKEW = 2
HOLD = 6
PIECES = 4
RS_CUTS = 2
HID_CUTS = 1


def spread(signal, kernel):
    padded = jnp.pad(signal, ((1, 1), (0, 0)))
    return padded[:-2] * kernel[0] + padded[1:-1] * kernel[1] + padded[2:] * kernel[2]


def activate(gate_sum, value_sum, kernel_gate, kernel_value, offset_gate, offset_value):
    gate_conv = spread(gate_sum, kernel_gate) + offset_gate
    value_conv = spread(value_sum, kernel_value) + offset_value
    return (jax.nn.silu(gate_conv) * value_conv).astype(jnp.bfloat16)


def plain_body(
    tokens,
    norm_gain,
    w_gate,
    w_value,
    conv_gate,
    conv_value,
    bias_gate,
    bias_value,
    w_down,
    out_gain,
):
    wide_in = tokens.astype(jnp.float32)
    width = wide_in.shape[1] * lax.axis_size("ra")
    squares = lax.psum(jnp.sum(wide_in * wide_in, axis=1), "ra")
    rscale = lax.rsqrt(squares / width + EPSILON)
    normed = (wide_in * rscale[:, None] * norm_gain.astype(jnp.float32)).astype(jnp.bfloat16)
    part_gate = jnp.dot(normed, w_gate, preferred_element_type=jnp.float32)
    part_value = jnp.dot(normed, w_value, preferred_element_type=jnp.float32)
    gate_sum, value_sum = (
        lax.psum_scatter(part_gate, "ra", scatter_dimension=1, tiled=True),
        lax.psum_scatter(part_value, "ra", scatter_dimension=1, tiled=True),
    )
    share_cols = gate_sum.shape[1]
    first_col = lax.axis_index("ra") * share_cols
    local_hidden = activate(
        gate_sum,
        value_sum,
        lax.dynamic_slice_in_dim(conv_gate, first_col, share_cols, 1),
        lax.dynamic_slice_in_dim(conv_value, first_col, share_cols, 1),
        lax.dynamic_slice_in_dim(bias_gate, first_col, share_cols, 0),
        lax.dynamic_slice_in_dim(bias_value, first_col, share_cols, 0),
    )
    partial_value = jnp.dot(
        lax.all_gather(local_hidden, "ra", axis=1, tiled=True),
        w_down,
        preferred_element_type=jnp.float32,
    )
    branch = lax.psum(partial_value, "cb")
    summed = RESIDUAL_WEIGHT * wide_in + branch
    totals = lax.psum(jnp.sum(summed * summed, axis=1), "ra")
    oscale = lax.rsqrt(totals / width + EPSILON)
    return (summed * oscale[:, None] * out_gain.astype(jnp.float32)).astype(jnp.bfloat16)


def to_row(column):
    rows = column.shape[0]
    return jnp.transpose(jnp.broadcast_to(column, (rows, LANES)))[:8]


def to_column(row):
    return jnp.transpose(jnp.broadcast_to(row, (LANES, row.shape[1])))[:, :1]


def shifted_sum(signal, taps, offset):
    rows = signal.shape[0]
    index = lax.broadcasted_iota(jnp.int32, signal.shape, 0)
    before = jnp.where(index == 0, 0.0, pltpu.roll(signal, 1, 0))
    after = jnp.where(index == rows - 1, 0.0, pltpu.roll(signal, rows - 1, 0))
    return before * taps[0:1] + signal * taps[1:2] + after * taps[2:3] + offset


def kernel(
    ra_size,
    tokens,
    norm_gain,
    w_gate,
    w_value,
    conv_gate,
    conv_value,
    bias_gate,
    bias_value,
    w_down,
    out_gain,
    out,
    w_in,
    w_out,
    normed,
    rs_out,
    rs_in,
    hid,
    part,
    acc,
    pair_in,
    x_out,
    x_in,
    summed,
    sq_col,
    sq_first,
    sq_last,
    w_in_sem,
    w_out_sem,
    rs_send,
    rs_recv,
    hid_send,
    hid_recv,
    pair_send,
    pair_recv,
    x_send,
    x_recv,
    sum_send,
    sum_recv,
    first_send,
    first_recv,
    last_send,
    last_recv,
):
    rows, wide = tokens.shape
    chunks = hid.shape[0]
    half = wide // 2
    width = wide * ra_size
    piece = rows // PIECES
    last = ra_size - 1

    me = lax.axis_index("ra")
    cb = lax.axis_index("cb")
    core = lax.rem(cb, 2)
    partner = cb + 1 - 2 * core
    across = lax.rem(cb + 2, 4)

    place = (me, last - me)
    ahead = (lax.rem(me + 1, ra_size), lax.rem(me + last, ra_size))
    behind = (ahead[1], ahead[0])
    lanes = (slice(LANES, 2 * LANES), slice(0, LANES))

    def w_in_copies(chunk):
        cols = pl.ds(pl.multiple_of(chunk * LANES, LANES), LANES)
        return [
            pltpu.make_async_copy(
                w.at[:, cols], w_in.at[chunk, :, n * LANES : (n + 1) * LANES], w_in_sem.at[n, chunk]
            )
            for n, w in enumerate((w_gate, w_value))
        ]

    def w_out_copies(k):
        return [
            pltpu.make_async_copy(
                w_down.at[pl.ds(pl.multiple_of((k + n * chunks) * LANES, LANES), LANES), :],
                w_out.at[k, n * LANES : (n + 1) * LANES, :],
                w_out_sem.at[n, k],
            )
            for n in range(2)
        ]

    def cut(c, cuts):
        return slice(c * rows // cuts, (c + 1) * rows // cuts)

    def rs_copy(d, k, c):
        return pltpu.make_async_remote_copy(
            src_ref=rs_out.at[d, k, cut(c, RS_CUTS)],
            dst_ref=rs_in.at[d, k, cut(c, RS_CUTS)],
            send_sem=rs_send.at[d, k, c],
            recv_sem=rs_recv.at[d, k, c],
            device_id={"ra": ahead[d]},
            device_id_type=MESH,
        )

    def hid_copy(d, k, c):
        return pltpu.make_async_remote_copy(
            src_ref=hid.at[k, cut(c, HID_CUTS), lanes[d]],
            dst_ref=hid.at[k, cut(c, HID_CUTS), lanes[d]],
            send_sem=hid_send.at[d, k, c],
            recv_sem=hid_recv.at[d, k, c],
            device_id={"ra": behind[d]},
            device_id_type=MESH,
        )

    barrier = pltpu.get_barrier_semaphore()
    for step in range(1, ra_size):
        for q in (cb, partner):
            pl.semaphore_signal(
                barrier, inc=1, device_id={"ra": lax.rem(me + step, ra_size), "cb": q}, device_id_type=MESH
            )
    for q in (partner, across):
        pl.semaphore_signal(barrier, inc=1, device_id={"cb": q}, device_id_type=MESH)

    @pl.loop(0, chunks)
    def _(k):
        for chunk in (k, k + chunks):
            for copy in w_in_copies(chunk):
                copy.start()

    @pl.loop(0, chunks)
    def _(k):
        for copy in w_out_copies(k):
            copy.start()

    wide_in = tokens[...].astype(jnp.float32)
    sq_first[me] = to_row(jnp.sum(wide_in * wide_in, axis=1, keepdims=True))
    acc[...] = jnp.zeros_like(acc)
    pl.semaphore_wait(barrier, 2 * last + 2)

    def first_copy(step):
        return pltpu.make_async_remote_copy(
            src_ref=sq_first.at[me],
            dst_ref=sq_first.at[me],
            send_sem=first_send.at[step],
            recv_sem=first_recv.at[me],
            device_id={"ra": lax.rem(me + step, ra_size)},
            device_id_type=MESH,
        )

    for step in range(1, ra_size):
        first_copy(step).start()
    for step in range(1, ra_size):
        source = lax.rem(me + step, ra_size)
        pltpu.make_async_remote_copy(
            src_ref=sq_first.at[source],
            dst_ref=sq_first.at[source],
            send_sem=first_send.at[step],
            recv_sem=first_recv.at[source],
            device_id={"ra": source},
            device_id_type=MESH,
        ).wait_recv()
    squares = sq_first[0, 0:1]
    for n in range(1, ra_size):
        squares = squares + sq_first[n, 0:1]
    rscale = lax.rsqrt(to_column(squares) / width + EPSILON)
    normed[...] = (tokens[...].astype(jnp.float32) * rscale * norm_gain[...].astype(jnp.float32)[None, :]).astype(
        jnp.bfloat16
    )

    def reduce_step(d, k):
        chunk = k + chunks if d == 0 else k
        for copy in w_in_copies(chunk):
            copy.wait()
        part[d] = jnp.dot(normed[...], w_in[chunk], preferred_element_type=jnp.float32)

        @pl.when(place[d] == 0)
        def _():
            for c in range(RS_CUTS):
                at = cut(c, RS_CUTS)
                rs_out[d, k, at] = part[d, at].astype(jnp.bfloat16)
                rs_copy(d, k, c).start()

        @pl.when((place[d] > 0) & (place[d] < last))
        def _():
            for c in range(RS_CUTS):
                at = cut(c, RS_CUTS)
                rs_copy(d, k, c).wait_recv()
                rs_out[d, k, at] = (part[d, at] + rs_in[d, k, at].astype(jnp.float32)).astype(jnp.bfloat16)
                rs_copy(d, k, c).start()

        @pl.when(place[d] == last)
        def _():
            for c in range(RS_CUTS):
                rs_copy(d, k, c).wait_recv()
            total = part[d] + rs_in[d, k].astype(jnp.float32)
            cols = pl.ds(pl.multiple_of(chunk * LANES, LANES), LANES)
            gate = shifted_sum(total[:, :LANES], conv_gate[:, cols], bias_gate[cols][None, :])
            value = shifted_sum(total[:, LANES:], conv_value[:, cols], bias_value[cols][None, :])
            hid[k, :, lanes[d]] = (gate / (1.0 + jnp.exp(-gate)) * value).astype(jnp.bfloat16)
            for c in range(HID_CUTS):
                hid_copy(d, k, c).start()

    def down_step(k):
        for copy in w_out_copies(k):
            copy.wait()
        for n in range(2):
            acc[n] += jnp.dot(
                hid[k], w_out[k, :, n * half : (n + 1) * half], preferred_element_type=jnp.float32
            )

    delay = LEAD + SKEW * (last - 1) + HOLD

    @pl.loop(0, chunks + delay + SKEW * (last - 1))
    def _(i):
        for d in range(2):
            k = i - jnp.where(place[d] == 0, 0, LEAD + SKEW * (place[d] - 1))
            pl.when((k >= 0) & (k < chunks))(functools.partial(reduce_step, d, k))
        for d in range(2):
            k = i - delay - SKEW * (last - 1 - place[d])

            @pl.when((k >= 0) & (k < chunks) & (place[d] < last))
            def _():
                for c in range(HID_CUTS):
                    hid_copy(d, k, c).wait_recv()

                    @pl.when(place[d] > 0)
                    def _():
                        hid_copy(d, k, c).start()

        k = i - delay - SKEW * (jnp.maximum(place[0], place[1]) - 1)
        pl.when((k >= 0) & (k < chunks))(functools.partial(down_step, k))

    def rows_of(p):
        return pl.ds(p * piece, piece)

    def pair_copy(p):
        return pltpu.make_async_remote_copy(
            src_ref=acc.at[1 - core, rows_of(p)],
            dst_ref=pair_in.at[rows_of(p)],
            send_sem=pair_send.at[p],
            recv_sem=pair_recv.at[p],
            device_id={"cb": partner},
            device_id_type=MESH,
        )

    def x_copy(p):
        return pltpu.make_async_remote_copy(
            src_ref=x_out.at[rows_of(p)],
            dst_ref=x_in.at[rows_of(p)],
            send_sem=x_send.at[p],
            recv_sem=x_recv.at[p],
            device_id={"cb": across},
            device_id_type=MESH,
        )

    def sum_copy(p, n):
        return pltpu.make_async_remote_copy(
            src_ref=summed.at[n, rows_of(p)],
            dst_ref=summed.at[n, rows_of(p)],
            send_sem=sum_send.at[p],
            recv_sem=sum_recv.at[p],
            device_id={"cb": partner},
            device_id_type=MESH,
        )

    def last_copy(owner, n, ra, q):
        return pltpu.make_async_remote_copy(
            src_ref=sq_last.at[owner],
            dst_ref=sq_last.at[owner],
            send_sem=last_send.at[n],
            recv_sem=last_recv.at[owner],
            device_id={"ra": ra, "cb": q},
            device_id_type=MESH,
        )

    for p in range(PIECES):
        pair_copy(p).start()
    for p in range(PIECES):
        pair_copy(p).wait_recv()
        x_out[rows_of(p), :] = (acc[core, rows_of(p)] + pair_in[rows_of(p), :]).astype(jnp.bfloat16)
        x_copy(p).start()
    own_cols = pl.ds(pl.multiple_of(core * half, LANES), half)
    for p in range(PIECES):
        x_copy(p).wait_recv()
        branch = x_out[rows_of(p), :].astype(jnp.float32) + x_in[rows_of(p), :].astype(jnp.float32)
        total = RESIDUAL_WEIGHT * tokens[rows_of(p), own_cols].astype(jnp.float32) + branch
        summed[core, rows_of(p)] = total
        sum_copy(p, core).start()
        sq_col[rows_of(p), :] = jnp.broadcast_to(jnp.sum(total * total, axis=1, keepdims=True), (piece, LANES))

    mine = 2 * me + core
    sq_last[mine] = jnp.transpose(sq_col[...])[:8]
    targets = [(me, partner)]
    for step in range(1, ra_size):
        targets += [(lax.rem(me + step, ra_size), q) for q in (cb, partner)]
    for n, (ra, q) in enumerate(targets):
        last_copy(mine, n, ra, q).start()
    for p in range(PIECES):
        sum_copy(p, 1 - core).wait_recv()
    for n, (ra, q) in enumerate(targets):
        last_copy(2 * ra + lax.rem(q, 2), n, ra, q).wait_recv()
    totals = sq_last[0, 0:1]
    for n in range(1, 2 * ra_size):
        totals = totals + sq_last[n, 0:1]
    oscale = lax.rsqrt(to_column(totals) / width + EPSILON)
    for n in range(2):
        cols = slice(n * half, (n + 1) * half)
        out[:, cols] = (summed[n] * oscale * out_gain[cols].astype(jnp.float32)[None, :]).astype(jnp.bfloat16)

    for step in range(1, ra_size):
        first_copy(step).wait_send()
    for d in range(2):

        @pl.loop(0, chunks)
        def _(k):
            @pl.when(place[d] < last)
            def _():
                for c in range(RS_CUTS):
                    rs_copy(d, k, c).wait_send()

            @pl.when(place[d] > 0)
            def _():
                for c in range(HID_CUTS):
                    hid_copy(d, k, c).wait_send()

    for p in range(PIECES):
        pair_copy(p).wait_send()
        x_copy(p).wait_send()
        sum_copy(p, core).wait_send()
    for n, (ra, q) in enumerate(targets):
        last_copy(mine, n, ra, q).wait_send()


def fused_body(
    tokens,
    norm_gain,
    w_gate,
    w_value,
    conv_gate,
    conv_value,
    bias_gate,
    bias_value,
    w_down,
    out_gain,
):
    ra_size = lax.axis_size("ra")
    rows, wide = tokens.shape
    chunks = w_gate.shape[1] // (2 * LANES)
    vmem = pl.BlockSpec(memory_space=pltpu.VMEM)
    anywhere = pl.BlockSpec(memory_space=pl.ANY)
    f32, bf16 = jnp.float32, jnp.bfloat16
    dma = pltpu.SemaphoreType.DMA
    return pl.pallas_call(
        functools.partial(kernel, ra_size),
        out_shape=jax.ShapeDtypeStruct((rows, wide), bf16),
        in_specs=[vmem, vmem, anywhere, anywhere, vmem, vmem, vmem, vmem, anywhere, vmem],
        out_specs=vmem,
        scratch_shapes=[
            pltpu.VMEM((2 * chunks, wide, 2 * LANES), bf16),
            pltpu.VMEM((chunks, 2 * LANES, wide), bf16),
            pltpu.VMEM((rows, wide), bf16),
            pltpu.VMEM((2, chunks, rows, 2 * LANES), bf16),
            pltpu.VMEM((2, chunks, rows, 2 * LANES), bf16),
            pltpu.VMEM((chunks, rows, 2 * LANES), bf16),
            pltpu.VMEM((2, rows, 2 * LANES), f32),
            pltpu.VMEM((2, rows, wide // 2), f32),
            pltpu.VMEM((rows, wide // 2), f32),
            pltpu.VMEM((rows, wide // 2), bf16),
            pltpu.VMEM((rows, wide // 2), bf16),
            pltpu.VMEM((2, rows, wide // 2), f32),
            pltpu.VMEM((rows, LANES), f32),
            pltpu.VMEM((ra_size, 8, rows), f32),
            pltpu.VMEM((2 * ra_size, 8, rows), f32),
            dma((2, 2 * chunks)),
            dma((2, chunks)),
            dma((2, chunks, RS_CUTS)),
            dma((2, chunks, RS_CUTS)),
            dma((2, chunks, HID_CUTS)),
            dma((2, chunks, HID_CUTS)),
            dma((PIECES,)),
            dma((PIECES,)),
            dma((PIECES,)),
            dma((PIECES,)),
            dma((PIECES,)),
            dma((PIECES,)),
            dma((ra_size,)),
            dma((ra_size,)),
            dma((2 * ra_size,)),
            dma((2 * ra_size,)),
        ],
        compiler_params=pltpu.CompilerParams(
            collective_id=0, has_side_effects=True, vmem_limit_bytes=56 * 1024 * 1024
        ),
    )(
        tokens,
        norm_gain,
        w_gate,
        w_value,
        conv_gate,
        conv_value,
        bias_gate,
        bias_value,
        w_down,
        out_gain,
    )


def solution(mesh):
    ra_size, cb_size = mesh.shape["ra"], mesh.shape["cb"]

    def body(*args):
        rows, wide = args[0].shape
        hidden = args[2].shape[1]
        fits = (
            ra_size >= 2
            and cb_size == 4
            and rows % LANES == 0
            and wide % (2 * LANES) == 0
            and hidden % (2 * LANES) == 0
            and 3 * 2 * wide * hidden + 10 * rows * hidden + 20 * rows * wide < 48 * 1024 * 1024
        )
        return fused_body(*args) if fits else plain_body(*args)

    return jax.shard_map(
        body,
        mesh=mesh,
        in_specs=(
            P("grp", "ra"),
            P("ra"),
            P("ra", "cb"),
            P("ra", "cb"),
            P(None, "cb"),
            P(None, "cb"),
            P("cb"),
            P("cb"),
            P("cb", "ra"),
            P("ra"),
        ),
        out_specs=P("grp", "ra"),
        check_vma=False,
    )
```
